256 devices in a mesh: rep: 2 (over z_hi), fs: 16 (over z_lo, y), tp: 8 (over x, core).
Axes of the slice: x: 4, y: 4, z: 8 (z_hi: 2, z_lo: 4; z = z_hi * 4 + z_lo), core: 2. Of those that a mesh axis runs over, the one named last changes fastest.
Arguments:
- tokens: bfloat16 [32768, 2048], P(('rep', 'fs', 'tp')), may hold values from -6 to 6
- mix_gain: float32 [2048], replicated, may hold values from 0.1 to 1.9
- query_weight: bfloat16 [2048, 2048], P('fs', 'tp'), may hold values from -0.125 to 0.125
- key_weight: bfloat16 [2048, 2048], P('fs', 'tp'), may hold values from -0.125 to 0.125
- value_weight: bfloat16 [2048, 2048], P('fs', 'tp'), may hold values from -0.125 to 0.125
- gate_weight: bfloat16 [2048, 2048], P('fs', 'tp'), may hold values from -0.125 to 0.125
- out_weight: bfloat16 [2048, 2048], P('fs', 'tp'), may hold values from -0.125 to 0.125
- head_gain: float32 [2048], replicated, may hold values from 0.1 to 1.9
- channel_gain: float32 [2048], replicated, may hold values from 0.1 to 1.9
- inner_gate: bfloat16 [2048, 6144], P('fs', 'tp'), may hold values from -0.125 to 0.125
- inner_lift: bfloat16 [2048, 6144], P('fs', 'tp'), may hold values from -0.125 to 0.125
- inner_down: bfloat16 [2048, 6144], P('fs', 'tp'), may hold values from -0.078125 to 0.078125
- filter_taps: float32 [3, 6144], replicated, may hold values from -3.5 to 3.5
- filter_bias: float32 [6144], replicated, may hold values from -3 to 3
Outputs:
- result: bfloat16 [32768, 2048], P(('rep', 'fs', 'tp'))
The draws below stay inside these ranges and needn't reach their ends.
All inputs are finite; a program needn't handle non-finite values.
Results may differ from the reference program's by a relative error of at most 0.017.
Values may be sent and summed in bfloat16 or wider, within the bound.
No kernel may reach another device: no remote copies, remote signals or barrier semaphores. Data moves between devices by JAX's collectives and lax.ppermute only.
A program may use at most 128 MiB of HBM per device.

```python
import jax
import jax.numpy as jnp
from jax import lax

D = 2048
HEADS = 8
HEAD_DIM = 256
FF = 6144
SEQ = 1024
BLOCK = 128
TAPS = 3
RW = 2048
TOKENS = 32768
N_TP = 8


def block_scale(rng, dims, shards, least, largest):
    def one(axis_at, shards_of):
        draws = jax.random.uniform(jax.random.fold_in(jax.random.fold_in(rng, 6), axis_at), (shards_of,), jnp.float32, least / len(shards), largest / len(shards))
        return jnp.repeat(jnp.exp(draws), dims[axis_at] // shards_of).reshape((-1,) + (1,) * (len(dims) - axis_at - 1))

    factor_of = one(*shards[0])
    for cut in shards[1:]:
        factor_of = factor_of * one(*cut)
    return factor_of


def noise(rng, shape, spread, limit, cuts=(), held_as=jnp.bfloat16):
    result = jax.random.normal(rng, shape, jnp.float32) * spread
    if len(cuts) > 0:
        result = block_scale(rng, shape, cuts, -0.22, 0.18) * result
    return jnp.clip(result, min=-limit, max=limit).astype(held_as)


def setup_inputs(seed: int = 0) -> dict:
    key_of = jax.random.split(jax.random.key(seed), 15)
    return {
        "tokens": noise(key_of[0], (TOKENS, D), 1.0, 6.0, ((0, 256),)),
        "mix_gain": jnp.clip(1.0 + 0.18 * jax.random.normal(key_of[1], (D,), jnp.float32), 0.1, 1.9),
        "query_weight": noise(key_of[2], (D, RW), D ** -0.5, 0.125, ((0, 16), (1, 8))),
        "key_weight": noise(key_of[3], (D, RW), D ** -0.5, 0.125, ((0, 16), (1, 8))),
        "value_weight": noise(key_of[4], (D, RW), D ** -0.5, 0.125, ((0, 16), (1, 8))),
        "gate_weight": noise(key_of[5], (D, RW), D ** -0.5, 0.125, ((0, 16), (1, 8))),
        "out_weight": noise(key_of[6], (D, RW), RW ** -0.5, 0.125, ((0, 16), (1, 8))),
        "head_gain": jnp.clip(1.0 + 0.18 * jax.random.normal(key_of[7], (RW,), jnp.float32), 0.1, 1.9),
        "channel_gain": jnp.clip(1.0 + 0.18 * jax.random.normal(key_of[8], (D,), jnp.float32), 0.1, 1.9),
        "inner_gate": noise(key_of[9], (D, FF), D ** -0.5, 0.125, ((0, 16), (1, 8))),
        "inner_lift": noise(key_of[10], (D, FF), D ** -0.5, 0.125, ((0, 16), (1, 8))),
        "inner_down": noise(key_of[11], (D, FF), FF ** -0.5, 0.078125, ((0, 16), (1, 8))),
        "filter_taps": noise(key_of[12], (TAPS, FF), TAPS ** -0.5, 3.5, (), jnp.float32),
        "filter_bias": noise(key_of[13], (FF,), 0.5, 3.0, (), jnp.float32),
    }


norm_eps = 1e-06
head_eps = 1.0
rope_base = 10000.0

def rms_scale(features, gain_row):
    mean_square = lax.optimization_barrier(jnp.mean(features * features, axis=-1, keepdims=True))
    return features * lax.rsqrt(mean_square + norm_eps) * gain_row

def rotate(heads_in, positions):
    half_width = heads_in.shape[-1] // 2
    inverse = rope_base ** (-jnp.arange(half_width, dtype=jnp.float32) / half_width)
    angles = positions[:, None] * inverse[None, :]
    cosine = jnp.cos(angles)[:, None, :]
    sine_part = jnp.sin(angles)[:, None, :]
    front_half = heads_in[..., :half_width]
    back_half = heads_in[..., half_width:]
    return jnp.concatenate([front_half * cosine - back_half * sine_part, front_half * sine_part + back_half * cosine], axis=-1)

def retain(queries, key_rows, value_rows, log_gamma, span):
    full_length, head_count, head_width = queries.shape
    blocks = full_length // span
    offsets = jnp.arange(span, dtype=jnp.float32)
    distance = offsets[:, None] - offsets[None, :]
    inside_segment_decay = jnp.where(distance[None] >= 0, jnp.exp(jnp.maximum(distance, 0.0)[None] * log_gamma[:, None, None]), 0.0)
    query_decay = jnp.exp((offsets[None, :] + 1.0) * log_gamma[:, None])
    key_decay_factor = jnp.exp((span - 1.0 - offsets[None, :]) * log_gamma[:, None])
    span_decay = jnp.exp(span * log_gamma)

    def to_spans(array):
        return array.reshape(blocks, span, head_count, head_width).transpose(0, 2, 1, 3)

    def advance(carry_state, inputs):
        query_segment, key_segment, value_span = inputs
        query_wide_precision = query_segment.astype(jnp.float32)
        key_wide_precision = key_segment.astype(jnp.float32)
        value_wide_precision = value_span.astype(jnp.float32)
        attention_scores = jnp.einsum('pol,pel->poe', query_wide_precision, key_wide_precision, precision=lax.Precision.HIGHEST) * inside_segment_decay
        span_weights = attention_scores.astype(jnp.bfloat16).astype(jnp.float32)
        within_span = jnp.einsum('hnm,hme->hne', span_weights, value_wide_precision, precision=lax.Precision.HIGHEST)
        carried = jnp.einsum('hnd,hde->hne', query_wide_precision, carry_state, precision=lax.Precision.HIGHEST) * query_decay[:, :, None]
        state_update = jnp.einsum('lqc,lqu->lcu', key_wide_precision * key_decay_factor[:, :, None], value_wide_precision, precision=lax.Precision.HIGHEST)
        return (carry_state * span_decay[:, None, None] + state_update, within_span + carried)
    initial = jnp.zeros((head_count, head_width, head_width), jnp.float32)
    unused, outputs = lax.scan(advance, initial, (to_spans(queries), to_spans(key_rows), to_spans(value_rows)))
    return outputs.transpose(0, 2, 1, 3).reshape(full_length, head_count, head_width)

def project(normed, weight):
    return jnp.dot(normed, weight, preferred_element_type=jnp.float32).astype(jnp.bfloat16)

def group_sum(hidden, weight, groups):
    seq_rows, columns = hidden.shape
    part_hidden = hidden.reshape(seq_rows, groups, columns // groups).astype(jnp.float32)
    part_weight = weight.reshape(weight.shape[0], groups, columns // groups).astype(jnp.float32)
    partial_value = jnp.einsum('sgc,dgc->gsd', part_hidden, part_weight, precision=lax.Precision.HIGHEST)
    rounded = lax.optimization_barrier(partial_value.astype(jnp.bfloat16))
    return lax.optimization_barrier(jnp.sum(rounded.astype(jnp.float32), axis=0))

def reference(tokens, mix_gain, query_weight, key_weight, value_weight, gate_weight, out_weight, head_gain, channel_gain, inner_gate, inner_lift, inner_down, filter_taps, filter_bias):
    head_ids = jnp.arange(HEADS, dtype=jnp.float32)
    log_gamma = jnp.log(1.0 - 2.0 ** (-5.0 - head_ids))
    positions = jnp.arange(SEQ, dtype=jnp.float32)

    def one_sequence(seq_rows):
        normed_in = rms_scale(seq_rows.astype(jnp.float32), mix_gain).astype(jnp.bfloat16)
        queries = project(normed_in, query_weight)
        key_rows = project(normed_in, key_weight)
        value_rows = project(normed_in, value_weight)
        gate_in = project(normed_in, gate_weight)
        q_rot = (rotate(queries.astype(jnp.float32).reshape(SEQ, HEADS, HEAD_DIM), positions) * HEAD_DIM ** (-0.5)).astype(jnp.bfloat16)
        k_rot = rotate(key_rows.astype(jnp.float32).reshape(SEQ, HEADS, HEAD_DIM), positions).astype(jnp.bfloat16)
        retained = retain(q_rot, k_rot, value_rows.reshape(SEQ, HEADS, HEAD_DIM), log_gamma, BLOCK)
        mean_square = lax.optimization_barrier(jnp.mean(retained * retained, axis=-1, keepdims=True))
        head_normed = (retained * lax.rsqrt(mean_square + head_eps)).reshape(SEQ, HEADS * HEAD_DIM) * head_gain
        mixed = (jax.nn.silu(gate_in.astype(jnp.float32)) * head_normed).astype(jnp.bfloat16)
        middle = seq_rows.astype(jnp.float32) + group_sum(mixed, out_weight, N_TP)
        normed_mid = rms_scale(middle, channel_gain).astype(jnp.bfloat16)
        gate_pre = project(normed_mid, inner_gate)
        lifted = project(normed_mid, inner_lift)
        padded = jnp.pad(gate_pre.astype(jnp.float32), ((TAPS - 1, 0), (0, 0)))
        filtered = filter_bias[None, :]
        for offset in range(TAPS):
            filtered = filtered + padded[offset:offset + SEQ] * filter_taps[offset][None, :]
        hidden = (jax.nn.silu(filtered) * lifted.astype(jnp.float32)).astype(jnp.bfloat16)
        return (middle + group_sum(hidden, inner_down, N_TP)).astype(jnp.bfloat16)
    sequences = tokens.reshape(TOKENS // SEQ, SEQ, D)
    return lax.map(one_sequence, sequences).reshape(TOKENS, D)
```

```python
import functools

import jax
import jax.numpy as jnp
from jax import lax
from jax.sharding import Mesh
from jax.sharding import PartitionSpec as P

HEAD_DIM = 256
BLOCK = 128
TAPS = 3
norm_eps = 1e-06
head_eps = 1.0
rope_base = 10000.0

OFFSETS = (0, -1, 1, 2)


def shift(array, axis, step):
    if axis == "z":
        axes = ("rep", "z")
        n = lax.axis_size("rep") * lax.axis_size("z")
    else:
        axes, n = axis, lax.axis_size(axis)
    return lax.ppermute(array, axes, [(i, (i + step) % n) for i in range(n)])


def ring_gather(own, axis):
    half = own.shape[0] // 2
    before = shift(own, axis, 1)
    after = shift(own, axis, -1)
    low = shift(before[:half], axis, 1)
    high = shift(after[half:], axis, -1)
    return [own, before, after, low, high]


def gather_weights(first, second):
    rows = first.shape[0]
    za = jnp.concatenate(ring_gather(first, "z"), axis=0)
    yb = jnp.concatenate(ring_gather(second, "y"), axis=0)
    all_a = jnp.concatenate(ring_gather(za, "y"), axis=0)
    all_b = jnp.concatenate(ring_gather(yb, "z"), axis=0)
    cols = all_b.shape[1]
    all_b = all_b.reshape(4, 4, rows, cols).transpose(1, 0, 2, 3).reshape(16 * rows, cols)
    return all_a, all_b


def gather_tokens(own):
    mine = jnp.concatenate(ring_gather(own, "x"), axis=0)
    return mine, shift(mine, "core", 1)


def scatter_sum(mine, partner):
    got = shift(partner, "core", 1)
    total = mine + got.astype(jnp.float32)
    half = total.shape[1] // 2
    far = total[3].astype(jnp.bfloat16)
    r1 = shift(far[:half], "x", 1)
    r2 = shift(far[half:], "x", -1)
    to_after = jnp.concatenate(
        [total[2, :half] + r1.astype(jnp.float32), total[2, half:]], axis=0
    ).astype(jnp.bfloat16)
    to_before = jnp.concatenate(
        [total[1, :half], total[1, half:] + r2.astype(jnp.float32)], axis=0
    ).astype(jnp.bfloat16)
    r3 = shift(to_after, "x", 1)
    r4 = shift(to_before, "x", -1)
    return total[0] + r3.astype(jnp.float32) + r4.astype(jnp.float32)


def rms_scale(features, gain_row):
    mean_square = jnp.mean(features * features, axis=-1, keepdims=True)
    return features * lax.rsqrt(mean_square + norm_eps) * gain_row


def rotate(heads_in, positions):
    half_width = heads_in.shape[-1] // 2
    inverse = rope_base ** (-jnp.arange(half_width, dtype=jnp.float32) / half_width)
    angles = positions[:, None] * inverse[None, :]
    cosine = jnp.cos(angles)
    sine_part = jnp.sin(angles)
    front_half = heads_in[..., :half_width]
    back_half = heads_in[..., half_width:]
    return jnp.concatenate(
        [front_half * cosine - back_half * sine_part, front_half * sine_part + back_half * cosine],
        axis=-1,
    )


def retain(queries, key_rows, value_rows, log_gamma):
    blocks, span, width = queries.shape
    offsets = jnp.arange(span, dtype=jnp.float32)
    distance = offsets[:, None] - offsets[None, :]
    decay = jnp.where(distance >= 0, jnp.exp(jnp.maximum(distance, 0.0) * log_gamma), 0.0)
    query_decay = jnp.exp((offsets + 1.0) * log_gamma)[:, None]
    key_decay = jnp.exp((span - 1.0 - offsets) * log_gamma)[:, None]
    span_decay = jnp.exp(span * log_gamma)

    def advance(state, inputs):
        q, k, v = inputs
        scores = lax.dot_general(q, k, (((1,), (1,)), ((), ())), preferred_element_type=jnp.float32)
        weights = (scores * decay).astype(jnp.bfloat16)
        within = jnp.dot(weights, v, preferred_element_type=jnp.float32)
        carried = jnp.dot(q.astype(jnp.float32), state) * query_decay
        update = lax.dot_general(
            k.astype(jnp.float32) * key_decay, v.astype(jnp.float32), (((0,), (0,)), ((), ()))
        )
        return state * span_decay + update, within + carried

    initial = jnp.zeros((width, width), jnp.float32)
    return lax.scan(advance, initial, (queries, key_rows, value_rows))[1]


def nt_dot(rows_in, weight):
    return lax.dot_general(
        rows_in, weight, (((1,), (1,)), ((), ())), preferred_element_type=jnp.float32
    )


def shards(
    tokens,
    mix_gain,
    query_weight,
    key_weight,
    value_weight,
    gate_weight,
    out_weight,
    head_gain,
    channel_gain,
    inner_gate,
    inner_lift,
    inner_down,
    filter_taps,
    filter_bias,
):
    x, core = lax.axis_index("x"), lax.axis_index("core")
    z, y = lax.axis_index("z"), lax.axis_index("y")
    tp_index = 2 * x + core
    rows, width = tokens.shape
    cols = query_weight.shape[1]
    hid = inner_gate.shape[1]
    chunk = width // 16
    offs = jnp.array(OFFSETS, jnp.int32)
    feature = (((z + offs) % 4)[None, :] * 4 + ((y + offs) % 4)[:, None]).reshape(16)
    span_of = (((x + offs) % 4)[None, :] * 2 + jnp.stack([core, 1 - core])[:, None]).reshape(8)
    place = jnp.array((0, 2, 3, 1), jnp.int32)
    four, two = jnp.arange(4), jnp.arange(2)
    place_of = (
        jnp.where(two == core, 0, 4)[None, :] + place[(four - x) % 4][:, None]
    ).reshape(8)
    feature_back = (
        4 * place[(four - y) % 4][None, :] + place[(four - z) % 4][:, None]
    ).reshape(16)

    def relative(a):
        return jnp.take(a.reshape(-1, 16, chunk), feature, axis=1).reshape(-1, width)

    half = cols // 2
    first = jnp.concatenate([query_weight, key_weight, out_weight[:, :half]], axis=1)
    second = jnp.concatenate([value_weight, gate_weight, out_weight[:, half:]], axis=1)
    mix_a, mix_b = gather_weights(first, second)
    tokens_rel = relative(tokens).astype(jnp.float32)
    normed_in = rms_scale(tokens_rel, relative(mix_gain)).astype(jnp.bfloat16)
    mine, partner = gather_tokens(normed_in)
    all_rows = jnp.concatenate([mine, partner], axis=0)
    full = all_rows.shape[0]
    qk = jnp.dot(all_rows, mix_a[:, : 2 * cols], preferred_element_type=jnp.float32)
    vg = jnp.dot(all_rows, mix_b[:, : 2 * cols], preferred_element_type=jnp.float32)
    out_w = jnp.concatenate([mix_a[:, 2 * cols :], mix_b[:, 2 * cols :]], axis=1)

    hfirst = jnp.concatenate([inner_gate, inner_down[:, : hid // 2]], axis=1)
    hsecond = jnp.concatenate([inner_lift, inner_down[:, hid // 2 :]], axis=1)
    ch_a, ch_b = gather_weights(hfirst, hsecond)

    def in_order(a):
        return jnp.take(a.reshape(8, rows, a.shape[-1]), place_of, axis=0)

    qk = in_order(qk.astype(jnp.bfloat16)).astype(jnp.float32)
    vg = in_order(vg.astype(jnp.bfloat16))
    positions = jnp.arange(full, dtype=jnp.float32)
    q_rot = (rotate(qk[..., :cols].reshape(full, cols), positions) * HEAD_DIM ** (-0.5)).astype(
        jnp.bfloat16
    )
    k_rot = rotate(qk[..., cols:].reshape(full, cols), positions).astype(jnp.bfloat16)
    log_gamma = jnp.log(1.0 - 2.0 ** (-5.0 - tp_index.astype(jnp.float32)))
    retained = retain(
        q_rot.reshape(8, rows, cols), k_rot.reshape(8, rows, cols), vg[..., :cols], log_gamma
    )
    mean_square = jnp.mean(retained * retained, axis=-1, keepdims=True)
    gain_dev = lax.dynamic_slice_in_dim(head_gain, tp_index * cols, cols, 0)
    head_normed = retained * lax.rsqrt(mean_square + head_eps) * gain_dev
    mixed = (jax.nn.silu(vg[..., cols:].astype(jnp.float32)) * head_normed).astype(jnp.bfloat16)
    mixed = jnp.take(mixed, span_of, axis=0).reshape(full, cols)
    part_out = nt_dot(mixed[full // 2 :], out_w).astype(jnp.bfloat16).reshape(4, rows, width)
    mine_out = nt_dot(mixed[: full // 2], out_w).reshape(4, rows, width)
    middle = tokens_rel + scatter_sum(mine_out, part_out)
    normed_mid = rms_scale(middle, relative(channel_gain)).astype(jnp.bfloat16)
    mine, partner = gather_tokens(normed_mid)
    all_rows = jnp.concatenate([mine, partner], axis=0)
    gate_pre = jnp.dot(all_rows, ch_a[:, :hid], preferred_element_type=jnp.float32)
    lifted = jnp.dot(all_rows, ch_b[:, :hid], preferred_element_type=jnp.float32)
    gate_pre = in_order(gate_pre.astype(jnp.bfloat16)).reshape(full, hid)
    lifted = in_order(lifted.astype(jnp.bfloat16)).reshape(full, hid)
    taps_dev = lax.dynamic_slice_in_dim(filter_taps, tp_index * hid, hid, 1)
    bias_dev = lax.dynamic_slice_in_dim(filter_bias, tp_index * hid, hid, 0)
    padded = jnp.pad(gate_pre.astype(jnp.float32), ((TAPS - 1, 0), (0, 0)))
    filtered = bias_dev[None, :]
    for offset in range(TAPS):
        filtered = filtered + padded[offset : offset + full] * taps_dev[offset][None, :]
    hidden = (jax.nn.silu(filtered) * lifted.astype(jnp.float32)).astype(jnp.bfloat16)
    hidden = jnp.take(hidden.reshape(8, rows, hid), span_of, axis=0).reshape(full, hid)
    down_w = jnp.concatenate([ch_a[:, hid:], ch_b[:, hid:]], axis=1)
    part_down = nt_dot(hidden[full // 2 :], down_w).astype(jnp.bfloat16).reshape(4, rows, width)
    mine_down = nt_dot(hidden[: full // 2], down_w).reshape(4, rows, width)
    outcome = (middle + scatter_sum(mine_down, part_down)).astype(jnp.bfloat16)
    return jnp.take(outcome.reshape(rows, 16, chunk), feature_back, axis=1).reshape(rows, width)


def solution(mesh):
    rep, fs, tp = (mesh.shape[a] for a in ("rep", "fs", "tp"))
    torus = Mesh(mesh.devices.reshape(rep, 4, fs // 4, tp // 2, 2), ("rep", "z", "y", "x", "core"))
    tok, fsa, tpa = P(("rep", "z", "y", "x", "core"), None), ("z", "y"), ("x", "core")
    w = P(fsa, tpa)
    in_specs = (tok, P(), w, w, w, w, w, P(), P(), w, w, w, P(), P())
    return jax.shard_map(shards, mesh=torus, in_specs=in_specs, out_specs=tok, check_vma=False)
```

```python
import functools

import jax
import jax.numpy as jnp
from jax import lax
from jax.experimental import pallas as pl
from jax.experimental.pallas import tpu as pltpu
from jax.sharding import Mesh
from jax.sharding import PartitionSpec as P

HEAD_DIM = 256
BLOCK = 128
TAPS = 3
norm_eps = 1e-06
head_eps = 1.0
rope_base = 10000.0
F32, BF16 = jnp.float32, jnp.bfloat16
VMEM = pl.BlockSpec(memory_space=pltpu.VMEM)
SMEM = pl.BlockSpec(memory_space=pltpu.SMEM)
PARAMS = pltpu.CompilerParams(vmem_limit_bytes=56 * 1024 * 1024)

SWAP1 = (0, 2, 1, 3)
SWAP = tuple(4 * SWAP1[i // 4] + SWAP1[i % 4] for i in range(16))
TURN = tuple(4 * (i % 4) + i // 4 for i in range(16))


def shift(array, axis, step):
    axes = ("rep", "z", "core") if axis == "z" else (axis, "core")
    n = 1
    for a in axes[:-1]:
        n *= lax.axis_size(a)
    pairs = []
    for i in range(n):
        for c, s in ((0, step), (1, -step)):
            pairs.append((2 * i + c, 2 * ((i + s) % n) + c))
    return lax.ppermute(array, axes, pairs)


def swap_core(array):
    return lax.ppermute(array, "core", [(0, 1), (1, 0)])


def ring_gather(own, axis):
    before = shift(own, axis, 1)
    after = shift(own, axis, -1)
    return [own, before, after, shift(before, axis, 1)]


def stack_kernel(*refs):
    out = refs[-1]
    rows = refs[0].shape[0]
    for i, r in enumerate(refs[:-1]):
        out[i * rows : (i + 1) * rows, :] = r[...]


def stacked(parts):
    rows, cols = parts[0].shape
    return pl.pallas_call(
        stack_kernel,
        out_shape=jax.ShapeDtypeStruct((rows * len(parts), cols), parts[0].dtype),
        in_specs=[VMEM] * len(parts),
        out_specs=VMEM,
        name="stack",
    )(*parts)


def norm_kernel(feature, tokens, gain, out):
    t = tokens[...].astype(F32)
    scale = lax.rsqrt(jnp.mean(t * t, axis=-1, keepdims=True) + norm_eps)
    for i in range(16):
        at = pl.ds(pl.multiple_of(feature[i] * 128, 128), 128)
        out[:, i * 128 : (i + 1) * 128] = (
            tokens[:, at].astype(F32) * scale * gain[:, at]
        ).astype(BF16)


def fill_rows(span_of, parts, rows_in):
    for j in range(4):
        rows_in[pl.ds(pl.multiple_of(span_of[j] * BLOCK, BLOCK), BLOCK), :] = parts[j][...]
    for j in range(4):
        at = pl.ds(pl.multiple_of(span_of[4 + j] * BLOCK, BLOCK), BLOCK)
        for i in range(16):
            rows_in[at, i * 128 : (i + 1) * 128] = parts[4 + j][
                :, SWAP[i] * 128 : (SWAP[i] + 1) * 128
            ]


def turned(block):
    return jnp.concatenate([block[:, 128 * i : 128 * i + 128] for i in TURN], axis=1)


def product(rows, parts, lo, hi):
    depth = parts[0].shape[0]
    total = None
    for i, p in enumerate(parts):
        one = jnp.dot(
            rows[:, i * depth : (i + 1) * depth], p[:, lo:hi], preferred_element_type=F32
        )
        total = one if total is None else total + one
    return total


def nt(a, b):
    return lax.dot_general(a, b, (((1,), (1,)), ((), ())), preferred_element_type=F32)


def tn(a, b):
    return lax.dot_general(a, b, (((0,), (0,)), ((), ())), preferred_element_type=F32)


def put_rows(place, step, core, left, right, parts_a, parts_b, lo, cut, mine, partner, hold):
    depth = parts_a[0].shape[0]
    for i in range(4):
        hold[:, i * depth : (i + 1) * depth] = nt(left, parts_a[i][:, lo : lo + cut[0]])
    for i in range(4):
        one = nt(right, parts_b[i][:, lo : lo + cut[1]])
        for k in range(4):
            at = 128 * TURN[4 * i + k]
            hold[:, at : at + 128] += one[:, 128 * k : 128 * k + 128]
    at = pl.ds(pl.multiple_of(core * BLOCK, BLOCK), BLOCK)
    mine[place[2 * step + core]] = hold[at, :]
    at = pl.ds(pl.multiple_of((1 - core) * BLOCK, BLOCK), BLOCK)
    to = place[2 * step + 1 - core] - 4
    for i in range(16):
        partner[to, :, i * 128 : (i + 1) * 128] = hold[
            at, SWAP[i] * 128 : (SWAP[i] + 1) * 128
        ].astype(BF16)


def mixer_kernel(*refs):
    span_of, place, core_ref = refs[:3]
    parts, wa, wb = refs[3:11], refs[11:15], refs[15:19]
    cosine, sine, decay, query_decay, key_decay, span_decay, gain = refs[19:26]
    mine, partner = refs[26:28]
    rows_in, state, hold = refs[28:]
    core = core_ref[0]
    fill_rows(span_of, parts, rows_in)
    state[...] = jnp.zeros_like(state)

    def step(t, carry):
        rows = rows_in[pl.ds(pl.multiple_of(t * 256, 256), 256), :]
        qk = product(rows, wa, 0, 512).astype(BF16).astype(F32)
        vg = product(turned(rows), wb, 0, 512).astype(BF16)
        at = pl.ds(pl.multiple_of(t * 256, 256), 256)
        c, s = cosine[at, :], sine[at, :]
        q1, q2, k1, k2 = (qk[:, 128 * i : 128 * i + 128] for i in range(4))
        q = (
            jnp.concatenate([q1 * c - q2 * s, q1 * s + q2 * c], axis=1) * HEAD_DIM ** (-0.5)
        ).astype(BF16)
        kf = jnp.concatenate([k1 * c - k2 * s, k1 * s + k2 * c], axis=1).astype(BF16)
        outs = []
        for u in range(2):
            lo, hi = u * BLOCK, (u + 1) * BLOCK
            qs, ks, vs = q[lo:hi], kf[lo:hi], vg[lo:hi, :HEAD_DIM]
            weights = (nt(qs, ks) * decay[...]).astype(BF16)
            held = state[...]
            out = jnp.dot(weights, vs, preferred_element_type=F32)
            out += jnp.dot(qs, held.astype(BF16), preferred_element_type=F32) * query_decay[...]
            decayed = (ks.astype(F32) * key_decay[...]).astype(BF16)
            state[...] = held * span_decay[...] + tn(decayed, vs)
            outs.append(out)
        retained = jnp.concatenate(outs, axis=0)
        scale = lax.rsqrt(jnp.mean(retained * retained, axis=-1, keepdims=True) + head_eps)
        g = vg[:, HEAD_DIM:].astype(F32)
        mixed = (g * jax.nn.sigmoid(g) * (retained * scale * gain[...])).astype(BF16)
        put_rows(
            place, t, core, mixed[:, :128], mixed[:, 128:], wa, wb, 512, (128, 128), mine,
            partner, hold,
        )
        return carry

    lax.fori_loop(0, 4, step, 0)


def channel_kernel(*refs):
    span_of, place, core_ref = refs[:3]
    parts, wa, wb = refs[3:11], refs[11:15], refs[15:19]
    taps, bias = refs[19:21]
    mine, partner = refs[21:23]
    rows_in, pre, hold = refs[23:]
    core = core_ref[0]
    hid = taps.shape[1]
    cut = (wa[0].shape[1] - hid, wb[0].shape[1] - hid)
    fill_rows(span_of, parts, rows_in)
    pre[0:8, :] = jnp.zeros((8, hid), F32)

    def step(t, carry):
        rows = rows_in[pl.ds(pl.multiple_of(t * 256, 256), 256), :]
        pre[8:264, :] = product(rows, wa, 0, hid).astype(BF16).astype(F32)
        lifted = product(turned(rows), wb, 0, hid).astype(BF16).astype(F32)
        filtered = bias[...] + pre[6:262, :] * taps[0:1, :]
        filtered += pre[7:263, :] * taps[1:2, :]
        filtered += pre[8:264, :] * taps[2:3, :]
        hidden = (filtered * jax.nn.sigmoid(filtered) * lifted).astype(BF16)
        pre[0:8, :] = pre[256:264, :]
        put_rows(
            place, t, core, hidden[:, : cut[0]], hidden[:, cut[0] :], wa, wb, hid, cut, mine,
            partner, hold,
        )
        return carry

    lax.fori_loop(0, 4, step, 0)


def middle_kernel(feature, tokens, gain, own, got, r3, r4, middle, normed):
    squares = jnp.zeros((tokens.shape[0], 1), F32)
    for i in range(16):
        lo, hi = i * 128, (i + 1) * 128
        at = pl.ds(pl.multiple_of(feature[i] * 128, 128), 128)
        m = tokens[:, at].astype(F32) + (
            (own[:, lo:hi] + got[:, lo:hi].astype(F32))
            + (r3[:, lo:hi].astype(F32) + r4[:, lo:hi].astype(F32))
        )
        middle[:, lo:hi] = m
        squares += jnp.sum(m * m, axis=-1, keepdims=True)
    scale = lax.rsqrt(squares / tokens.shape[1] + norm_eps)
    for i in range(16):
        lo, hi = i * 128, (i + 1) * 128
        at = pl.ds(pl.multiple_of(feature[i] * 128, 128), 128)
        normed[:, lo:hi] = (middle[:, lo:hi] * scale * gain[:, at]).astype(BF16)


def final_kernel(feature, middle, own, got, r3, r4, out):
    for i in range(16):
        lo, hi = i * 128, (i + 1) * 128
        at = pl.ds(pl.multiple_of(feature[i] * 128, 128), 128)
        out[:, at] = (
            middle[:, lo:hi]
            + (own[:, lo:hi] + got[:, lo:hi].astype(F32))
            + (r3[:, lo:hi].astype(F32) + r4[:, lo:hi].astype(F32))
        ).astype(BF16)


def add_kernel(own, got, out):
    out[...] = (own[...] + got[...].astype(F32)).astype(BF16)


def add3_kernel(own, got, more, out):
    out[...] = (own[...] + got[...].astype(F32) + more[...].astype(F32)).astype(BF16)


def small_call(kernel, name, outs, *args):
    return pl.pallas_call(
        kernel,
        out_shape=outs,
        in_specs=[SMEM if a.dtype == jnp.int32 else VMEM for a in args],
        out_specs=jax.tree.map(lambda _: VMEM, outs),
        compiler_params=PARAMS,
        name=name,
    )(*args)


def scatter_sum(mine, partner):
    rows, cols = mine.shape[1:]
    got = swap_core(partner)
    block = jax.ShapeDtypeStruct((rows, cols), BF16)
    far = small_call(add_kernel, "add_far", block, mine[3], got[3])
    passed = shift(far, "x", 1)
    before = small_call(add_kernel, "add_before", block, mine[1], got[1])
    r4 = shift(before, "x", -1)
    after = small_call(add3_kernel, "add_after", block, mine[2], got[2], passed)
    r3 = shift(after, "x", 1)
    return mine[0], got[0], r3, r4


def gather_weights(first, second):
    za = stacked(ring_gather(first, "z"))
    yb = stacked(ring_gather(second, "y"))
    return ring_gather(za, "y"), ring_gather(yb, "z")


def gather_tokens(own):
    mine = ring_gather(own, "x")
    return mine + [swap_core(m) for m in mine]


def shards(
    tokens,
    mix_gain,
    query_weight,
    key_weight,
    value_weight,
    gate_weight,
    out_weight,
    head_gain,
    channel_gain,
    inner_gate,
    inner_lift,
    inner_down,
    filter_taps,
    filter_bias,
):
    x, core = lax.axis_index("x"), lax.axis_index("core")
    z, y = lax.axis_index("z"), lax.axis_index("y")
    tp_index = 2 * x + core
    rows, width = tokens.shape
    cols = query_weight.shape[1]
    hid = inner_gate.shape[1]
    full = 8 * rows
    sign = 1 - 2 * core
    offs = [0, -sign, sign, 2]
    feature = jnp.stack(
        [((z + offs[i % 4]) % 4) * 4 + (y + offs[i // 4]) % 4 for i in range(16)]
    ).astype(jnp.int32)
    spans = [((x + offs[j]) % 4) * 2 + core for j in range(4)]
    spans += [((x + offs[SWAP1[j]]) % 4) * 2 + 1 - core for j in range(4)]
    span_of = jnp.stack(spans).astype(jnp.int32)
    place = jnp.sum(
        jnp.where(span_of[:, None] == jnp.arange(8)[None, :], jnp.arange(8)[:, None], 0), axis=0
    ).astype(jnp.int32)
    core_ref = core.reshape(1).astype(jnp.int32)

    half = cols // 2
    first = jnp.concatenate([query_weight, key_weight, out_weight[:, :half]], axis=1)
    second = jnp.concatenate([value_weight, gate_weight, out_weight[:, half:]], axis=1)
    down_cut = hid // 3
    hfirst = jnp.concatenate([inner_gate, inner_down[:, :down_cut]], axis=1)
    hsecond = jnp.concatenate([inner_lift, inner_down[:, down_cut:]], axis=1)

    block = jax.ShapeDtypeStruct((rows, width), BF16)
    wide = jax.ShapeDtypeStruct((rows, width), F32)
    normed_in = small_call(
        norm_kernel, "norm", block, feature, tokens, mix_gain.reshape(1, width)
    )
    pieces = gather_tokens(normed_in)
    wa, wb = gather_weights(first, second)

    positions = jnp.arange(full, dtype=F32)
    inverse = rope_base ** (-jnp.arange(HEAD_DIM // 2, dtype=F32) / (HEAD_DIM // 2))
    angles = positions[:, None] * inverse[None, :]
    log_gamma = jnp.log(1.0 - 2.0 ** (-5.0 - tp_index.astype(F32)))
    offsets = jnp.arange(BLOCK, dtype=F32)
    distance = offsets[:, None] - offsets[None, :]
    decay = jnp.where(distance >= 0, jnp.exp(jnp.maximum(distance, 0.0) * log_gamma), 0.0)
    query_decay = jnp.broadcast_to(
        jnp.exp((offsets + 1.0) * log_gamma)[:, None], (BLOCK, HEAD_DIM)
    )
    key_decay = jnp.broadcast_to(
        jnp.exp((BLOCK - 1.0 - offsets) * log_gamma)[:, None], (BLOCK, HEAD_DIM)
    )
    span_decay = jnp.full((1, HEAD_DIM), jnp.exp(BLOCK * log_gamma), F32)
    gain_dev = lax.dynamic_slice_in_dim(head_gain, tp_index * cols, cols, 0).reshape(1, cols)
    outs = (
        jax.ShapeDtypeStruct((4, rows, width), F32),
        jax.ShapeDtypeStruct((4, rows, width), BF16),
    )

    def big_call(kernel, name, scratch, *args):
        return pl.pallas_call(
            kernel,
            out_shape=outs,
            in_specs=[SMEM] * 3 + [VMEM] * len(args),
            out_specs=(VMEM, VMEM),
            scratch_shapes=[
                pltpu.VMEM((full, width), BF16),
                pltpu.VMEM(scratch, F32),
                pltpu.VMEM((256, width), F32),
            ],
            compiler_params=PARAMS,
            name=name,
        )(span_of, place, core_ref, *args)

    mine, partner = big_call(
        mixer_kernel, "mixer", (HEAD_DIM, HEAD_DIM), *pieces, *wa, *wb, jnp.cos(angles),
        jnp.sin(angles), decay, query_decay, key_decay, span_decay, gain_dev,
    )
    ca, cb = gather_weights(hfirst, hsecond)
    middle, normed_mid = small_call(
        middle_kernel, "middle", (wide, block), feature, tokens,
        channel_gain.reshape(1, width), *scatter_sum(mine, partner),
    )
    pieces = gather_tokens(normed_mid)
    taps_dev = lax.dynamic_slice_in_dim(filter_taps, tp_index * hid, hid, 1)
    bias_dev = lax.dynamic_slice_in_dim(filter_bias, tp_index * hid, hid, 0).reshape(1, hid)
    mine, partner = big_call(
        channel_kernel, "channel", (264, hid), *pieces, *ca, *cb, taps_dev, bias_dev
    )
    return small_call(
        final_kernel, "final", block, feature, middle, *scatter_sum(mine, partner)
    )


def solution(mesh):
    rep, fs, tp = (mesh.shape[a] for a in ("rep", "fs", "tp"))
    torus = Mesh(mesh.devices.reshape(rep, 4, fs // 4, tp // 2, 2), ("rep", "z", "y", "x", "core"))
    tok, fsa, tpa = P(("rep", "z", "y", "x", "core"), None), ("z", "y"), ("x", "core")
    w = P(fsa, tpa)
    in_specs = (tok, P(), w, w, w, w, w, P(), P(), w, w, w, P(), P())
    return jax.shard_map(shards, mesh=torus, in_specs=in_specs, out_specs=tok, check_vma=False)
```
